32 devices in a mesh: sp: 16 (over z, y, x), tp: 2 (over core).
Axes of the slice: x: 2, y: 2, z: 4, core: 2. Of those that a mesh axis runs over, the one named last changes fastest.
Arguments:
- residual: bfloat16 [3072, 2048], P(('sp', 'tp')), may hold values from -6 to 6
- queries_narrow: bfloat16 [3072, 512], P('sp', 'tp'), may hold values from -24 to 24
- keys_narrow: bfloat16 [3072, 512], P('sp', 'tp'), may hold values from -24 to 24
- values_narrow: bfloat16 [3072, 512], P('sp', 'tp'), may hold values from -6 to 6
- queries_broad: bfloat16 [3072, 512], P('sp', 'tp'), may hold values from -24 to 24
- keys_broad: bfloat16 [3072, 512], P('sp', 'tp'), may hold values from -24 to 24
- values_broad: bfloat16 [3072, 512], P('sp', 'tp'), may hold values from -6 to 6
- gates_narrow: float32 [3072, 16], P('sp', 'tp'), may hold values from -3072 to 0, as said below
- gates_broad: float32 [3072, 8], P('sp', 'tp'), may hold values from -3072 to 0, as said below
- project_narrow: bfloat16 [512, 2048], P('tp'), may hold values from -0.5 to 0.5
- project_broad: bfloat16 [512, 2048], P('tp'), may hold values from -0.5 to 0.5
- norm_gain: float32 [2048], replicated, may hold values from 0.1 to 1.9
- up_weight: bfloat16 [2048, 8192], P('sp', 'tp'), may hold values from -0.125 to 0.125
- down_weight: bfloat16 [8192, 2048], P('tp', 'sp'), may hold values from -0.0625 to 0.0625
Outputs:
- layer_out: bfloat16 [3072, 2048], P(('sp', 'tp'))
The draws below stay inside these ranges and needn't reach their ends.
Inputs may be any that keep to these rules, and one draw needn't show every extreme that they name: `gates_narrow`: each head's cumulative log gate never rises from one position to the next. `gates_broad`: each head's cumulative log gate never rises from one position to the next.
All inputs are finite; a program needn't handle non-finite values.
Results may differ from the reference program's by a relative error of at most 0.018.
Values may be sent and summed in bfloat16 or wider, within the bound.
A program may use at most 128 MiB of HBM per device.

```python
import jax
import jax.numpy as jnp
from jax import lax

D = 2048
FF = 8192
A_HEADS = 16
A_DIM = 32
B_HEADS = 8
B_DIM = 64
TOK_DEV = 192
CONTEXT_LENGTH = 3072


def paired_rows(key, width):
    key_query, key_keys = jax.random.split(key, 2)
    queries = jax.random.normal(key_query, (CONTEXT_LENGTH, width), jnp.float32)
    keys = jax.random.normal(key_keys, (CONTEXT_LENGTH, width), jnp.float32)
    return (queries.astype(jnp.bfloat16), keys.astype(jnp.bfloat16))


def draw_queries_narrow(key, part):
    return paired_rows(jax.random.fold_in(key, 11), A_HEADS * A_DIM)[0]


def draw_keys_narrow(key, part):
    return paired_rows(jax.random.fold_in(key, 11), A_HEADS * A_DIM)[1]


def draw_queries_broad(key, part):
    return paired_rows(jax.random.fold_in(key, 12), B_HEADS * B_DIM)[0]


def draw_keys_broad(key, part):
    return paired_rows(jax.random.fold_in(key, 12), B_HEADS * B_DIM)[1]


def forget_gates(key, heads):
    category_seed, quick_decay_seed, gradual_decay_seed, tile_seed, sample_seed, spike_seed, quantity_seed = jax.random.split(key, 7)
    slow_share = 0.5
    slow = jax.random.uniform(category_seed, (heads,), jnp.float32) < slow_share
    fast_rate = 1.0 / jax.random.uniform(quick_decay_seed, (heads,), jnp.float32, 30.0, 50.0)
    slow_rate = jax.random.uniform(gradual_decay_seed, (heads,), jnp.float32, 0.5, 1.0) / CONTEXT_LENGTH
    rate = jnp.where(slow, slow_rate, fast_rate)
    blocks = CONTEXT_LENGTH // TOK_DEV
    block_factor = jnp.exp(jax.random.uniform(tile_seed, (blocks,), jnp.float32, -0.7, 0.7))
    block_factor = jnp.repeat(block_factor, TOK_DEV)
    data_part = jnp.exp(jax.random.uniform(sample_seed, (CONTEXT_LENGTH, heads), jnp.float32, -1.2, 1.1))
    forget_log_factor = -rate[None, :] * block_factor[:, None] * data_part
    position_spike = jax.random.uniform(spike_seed, (CONTEXT_LENGTH, 1), jnp.float32) < 2.0 / CONTEXT_LENGTH
    position_quantity = jax.random.uniform(quantity_seed, (CONTEXT_LENGTH, heads), jnp.float32, 0.22, 0.69)
    forget_log_factor = forget_log_factor - jnp.where(position_spike, position_quantity, 0.0)
    return jnp.cumsum(forget_log_factor, axis=0)


def draw_gates_narrow(key, part):
    return forget_gates(jax.random.fold_in(key, 21), A_HEADS)


def draw_gates_broad(key, part):
    return forget_gates(jax.random.fold_in(key, 22), B_HEADS)


def block_scale(key, shape, cuts, low, high):
    gain, own = 1.0, jax.random.fold_in(key, 6)
    for dim, blocks in cuts:
        steps = jnp.exp(jax.random.uniform(jax.random.fold_in(own, dim), (blocks,), jnp.float32, low / len(cuts), high / len(cuts)))
        gain = gain * jnp.repeat(steps, shape[dim] // blocks).reshape([-1 if axis == dim else 1 for axis in range(len(shape))])
    return gain


def bell_draw(own_key, extent, spread, limit, cuts=(), kind=jnp.bfloat16):
    array = spread * jax.random.normal(own_key, extent, jnp.float32)
    if cuts:
        array = array * block_scale(own_key, extent, cuts, -0.22, 0.18)
    return jnp.clip(array, -limit, limit).astype(kind)


def setup_inputs(seed: int = 0) -> dict:
    streams_of = jax.random.split(jax.random.key(seed), 15)
    return {
        "residual": bell_draw(streams_of[0], (CONTEXT_LENGTH, D), 1.0, 6.0, ((0, 32),)),
        "queries_narrow": draw_queries_narrow(jax.random.fold_in(streams_of[14], 71), 0),
        "keys_narrow": draw_keys_narrow(jax.random.fold_in(streams_of[14], 71), 0),
        "values_narrow": bell_draw(streams_of[3], (CONTEXT_LENGTH, A_HEADS * A_DIM), 1.0, 6.0, ((0, 16), (1, 2))),
        "queries_broad": draw_queries_broad(jax.random.fold_in(streams_of[14], 71), 0),
        "keys_broad": draw_keys_broad(jax.random.fold_in(streams_of[14], 71), 0),
        "values_broad": bell_draw(streams_of[6], (CONTEXT_LENGTH, B_HEADS * B_DIM), 1.0, 6.0, ((0, 16), (1, 2))),
        "gates_narrow": draw_gates_narrow(jax.random.fold_in(streams_of[14], 71), 0),
        "gates_broad": draw_gates_broad(jax.random.fold_in(streams_of[14], 71), 0),
        "project_narrow": bell_draw(streams_of[9], (A_HEADS * A_DIM, D), ((A_HEADS * A_DIM + B_HEADS * B_DIM) // 8) ** -0.5, 0.5, ((0, 2),)),
        "project_broad": bell_draw(streams_of[10], (B_HEADS * B_DIM, D), ((A_HEADS * A_DIM + B_HEADS * B_DIM) // 8) ** -0.5, 0.5, ((0, 2),)),
        "norm_gain": jnp.clip(1.0 + 0.18 * jax.random.normal(streams_of[11], (D,), jnp.float32), 0.1, 1.9),
        "up_weight": bell_draw(streams_of[12], (D, FF), D ** -0.5, 0.125, ((0, 16), (1, 2))),
        "down_weight": bell_draw(streams_of[13], (FF, D), FF ** -0.5, 0.0625, ((0, 2), (1, 16))),
    }


def group_attention(queries, keys, values, gates, head_size):
    total_rows = queries.shape[0]
    heads = queries.shape[1] // head_size
    block = min(512, total_rows)
    blocks = total_rows // block
    query_blocks = queries.astype(jnp.float32).reshape(blocks, block, heads, head_size)
    gate_blocks = gates.reshape(blocks, block, heads)
    key_heads = keys.astype(jnp.float32).reshape(total_rows, heads, head_size)
    value_heads = values.astype(jnp.float32).reshape(total_rows, heads, head_size)
    key_pos = jnp.arange(total_rows, dtype=jnp.int32)

    def one_block(inputs):
        index, query_block, gate_block = inputs
        scores = jnp.einsum('qhd,khd->hqk', query_block, key_heads) * head_size ** (-0.5)
        scores = scores + gate_block.T[:, :, None] - gates.T[:, None, :]
        query_pos = index * block + jnp.arange(block, dtype=jnp.int32)
        allowed = key_pos[None, :] <= query_pos[:, None]
        scores = jnp.where(allowed[None], scores, -jnp.inf)
        peak = lax.optimization_barrier(jnp.max(scores, axis=-1, keepdims=True))
        weights = jnp.exp(scores - peak)
        denom = lax.optimization_barrier(jnp.sum(weights, axis=-1))
        summed = jnp.einsum('hqk,khd->hqd', weights.astype(jnp.bfloat16).astype(jnp.float32), value_heads)
        result = summed / denom[..., None]
        return result.transpose(1, 0, 2).reshape(block, heads * head_size)
    output = lax.map(one_block, (jnp.arange(blocks, dtype=jnp.int32), query_blocks, gate_blocks))
    return output.reshape(total_rows, heads * head_size).astype(jnp.bfloat16)

def reference(residual, queries_narrow, keys_narrow, values_narrow, queries_broad, keys_broad, values_broad, gates_narrow, gates_broad, project_narrow, project_broad, norm_gain, up_weight, down_weight):
    attended_narrow = group_attention(queries_narrow, keys_narrow, values_narrow, gates_narrow, A_DIM)
    attended_broad = group_attention(queries_broad, keys_broad, values_broad, gates_broad, B_DIM)
    projected = jnp.dot(attended_narrow, project_narrow, preferred_element_type=jnp.float32)
    projected = projected + jnp.dot(attended_broad, project_broad, preferred_element_type=jnp.float32)
    mixed = (residual.astype(jnp.float32) + projected).astype(jnp.bfloat16)
    mixed_wide = mixed.astype(jnp.float32)
    scale = lax.rsqrt(lax.optimization_barrier(jnp.mean(mixed_wide * mixed_wide, axis=-1, keepdims=True)) + 1e-06)
    normed = (mixed_wide * scale * norm_gain.astype(jnp.float32)).astype(jnp.bfloat16)
    hidden = jnp.square(jax.nn.relu(jnp.dot(normed, up_weight, preferred_element_type=jnp.float32))).astype(jnp.bfloat16)
    return (mixed_wide + jnp.dot(hidden, down_weight, preferred_element_type=jnp.float32)).astype(jnp.bfloat16)
```

```python
import functools

import jax
import jax.numpy as jnp
from jax import lax
from jax.experimental import pallas as pl
from jax.experimental.pallas import tpu as pltpu
from jax.sharding import PartitionSpec as P

A_DIM = 32
B_DIM = 64


def group_update(state, queries, keys, values, query_gates, key_gates, allowed, head_size):
    peak, total, summed = state
    query_count = queries.shape[0]
    key_count = keys.shape[0]
    heads = queries.shape[1] // head_size
    scores = jnp.einsum(
        "qhd,khd->hqk",
        queries.reshape(query_count, heads, head_size),
        keys.reshape(key_count, heads, head_size),
        preferred_element_type=jnp.float32,
    ) * head_size ** (-0.5)
    scores = scores + query_gates.T[:, :, None] - key_gates.T[:, None, :]
    scores = jnp.where(allowed[None], scores, -1e30)
    new_peak = jnp.maximum(peak, jnp.max(scores, axis=-1))
    weights = jnp.exp(scores - new_peak[..., None]) * allowed[None].astype(jnp.float32)
    total = jnp.sum(weights, axis=-1)
    summed = jnp.einsum(
        "hqk,khd->hqd",
        weights.astype(jnp.bfloat16),
        values.reshape(key_count, heads, head_size),
        preferred_element_type=jnp.float32,
    )
    return (new_peak, total, summed)


def empty_state(query_count, heads, head_size):
    return (
        jnp.full((heads, query_count), -1e30, jnp.float32),
        jnp.zeros((heads, query_count), jnp.float32),
        jnp.zeros((heads, query_count, head_size), jnp.float32),
    )


def finish_group(state, head_size):
    peak, total, summed = state
    result = summed / total[..., None]
    return (
        result.transpose(1, 0, 2)
        .reshape(result.shape[1], result.shape[0] * head_size)
        .astype(jnp.bfloat16)
    )


def rms_scaled(mixed, norm_gain):
    mixed_wide = mixed.astype(jnp.float32)
    scale = lax.rsqrt(jnp.mean(mixed_wide * mixed_wide, axis=-1, keepdims=True) + 1e-06)
    return (mixed_wide * scale * norm_gain).astype(jnp.bfloat16)


def group_size(sp_count):
    return 8 if sp_count % 8 == 0 else sp_count


def weights_kernel(
    count, group, up_ref, down_ref, up_out, down_out, up_hold, down_hold, sems, own_sems
):
    me = lax.axis_index("sp")
    up_rows = up_ref.shape[0]
    units = up_out.shape[1]
    columns = down_ref.shape[1]
    barrier = pltpu.get_barrier_semaphore()

    def hello(k, carry):
        pl.semaphore_signal(
            barrier,
            inc=1,
            device_id={"sp": (me + k) % count},
            device_id_type=pl.DeviceIdType.MESH,
        )
        return carry

    lax.fori_loop(1, count, hello, 0)
    pl.semaphore_wait(barrier, count - 1)

    def up_source(chunk):
        return up_ref.at[:, pl.ds(pl.multiple_of(chunk * units, 128), units)]

    def down_source(chunk):
        return down_ref.at[pl.ds(pl.multiple_of(chunk * units, units), units), :]

    def up_target(owner):
        return up_out.at[pl.ds(pl.multiple_of(owner * up_rows, up_rows), up_rows), :]

    def down_target(owner):
        if len(down_out.shape) == 3:
            return down_out.at[owner]
        return down_out.at[:, pl.ds(pl.multiple_of(owner * columns, columns), columns)]

    def copies(k, target_owner):
        peer = (me + k) % count
        chunk = peer % group
        pairs = (
            (up_source(chunk), up_target(target_owner)),
            (down_source(chunk), down_target(target_owner)),
        )
        return [
            pltpu.make_async_remote_copy(
                src_ref=source,
                dst_ref=target,
                send_sem=sems.at[0, which, k],
                recv_sem=sems.at[1, which, k],
                device_id={"sp": peer},
                device_id_type=pl.DeviceIdType.MESH,
            )
            for which, (source, target) in enumerate(pairs)
        ]

    def start(k, carry):
        for copy in copies(k, me):
            copy.start()
        return carry

    def finish(k, carry):
        for copy in copies(k, (me + count - k) % count):
            copy.wait_recv()
            copy.wait_send()
        return carry

    lax.fori_loop(1, count, start, 0)
    own = me % group
    first = [
        pltpu.make_async_copy(up_source(own), up_hold, own_sems.at[0]),
        pltpu.make_async_copy(down_source(own), down_hold, own_sems.at[1]),
    ]
    for copy in first:
        copy.start()
    for copy in first:
        copy.wait()
    second = [
        pltpu.make_async_copy(up_hold, up_target(me), own_sems.at[0]),
        pltpu.make_async_copy(down_hold, down_target(me), own_sems.at[1]),
    ]
    for copy in second:
        copy.start()
    for copy in second:
        copy.wait()
    lax.fori_loop(1, count, finish, 0)


def share_weights(up_weight, down_weight):
    count = lax.axis_size("sp")
    group = group_size(count)
    up_rows, unit_total = up_weight.shape
    columns = down_weight.shape[1]
    units = unit_total // group
    if columns % 128 == 0:
        down_shape = (units, count * columns)
    else:
        down_shape = (count, units, columns)
    up_full, down_full = pl.pallas_call(
        functools.partial(weights_kernel, count, group),
        out_shape=(
            jax.ShapeDtypeStruct((count * up_rows, units), up_weight.dtype),
            jax.ShapeDtypeStruct(down_shape, down_weight.dtype),
        ),
        in_specs=[pl.BlockSpec(memory_space=pl.ANY)] * 2,
        out_specs=[pl.BlockSpec(memory_space=pl.ANY)] * 2,
        scratch_shapes=[
            pltpu.VMEM((up_rows, units), up_weight.dtype),
            pltpu.VMEM((units, columns), down_weight.dtype),
            pltpu.SemaphoreType.DMA((2, 2, count)),
            pltpu.SemaphoreType.DMA((2,)),
        ],
        compiler_params=pltpu.CompilerParams(collective_id=0, has_side_effects=True),
        cost_estimate=pl.CostEstimate(
            flops=0, bytes_accessed=count * up_rows * units * 80, transcendentals=0
        ),
    )(up_weight, down_weight)
    if columns % 128:
        down_full = down_full.transpose(1, 0, 2).reshape(units, count * columns)
    return up_full, down_full


def gather_kernel(group, tp_count, rows_ref, out_ref, hold, sems, own_sems, pass_sems):
    sp = lax.axis_index("sp")
    tp = lax.axis_index("tp")
    base = (sp // group) * group
    me = sp - base
    barrier = pltpu.get_barrier_semaphore()
    for k in range(1, group):
        pl.semaphore_signal(
            barrier,
            inc=1,
            device_id={"sp": base + (me + k) % group},
            device_id_type=pl.DeviceIdType.MESH,
        )
    for j in range(1, tp_count):
        pl.semaphore_signal(
            barrier,
            inc=1,
            device_id={"tp": (tp + j) % tp_count},
            device_id_type=pl.DeviceIdType.MESH,
        )
    pl.semaphore_wait(barrier, group + tp_count - 2)

    def across(k, owner):
        return pltpu.make_async_remote_copy(
            src_ref=rows_ref,
            dst_ref=out_ref.at[tp, owner],
            send_sem=sems.at[0, k],
            recv_sem=sems.at[1, k],
            device_id={"sp": base + (me + k) % group},
            device_id_type=pl.DeviceIdType.MESH,
        )

    def beside(j, k, source, tp_owner, owner):
        return pltpu.make_async_remote_copy(
            src_ref=source,
            dst_ref=out_ref.at[tp_owner, owner],
            send_sem=pass_sems.at[0, j, k],
            recv_sem=pass_sems.at[1, j, k],
            device_id={"tp": (tp + j) % tp_count},
            device_id_type=pl.DeviceIdType.MESH,
        )

    for k in range(1, group):
        across(k, me).start()
    for j in range(1, tp_count):
        beside(j, 0, rows_ref, tp, me).start()
    own = pltpu.make_async_copy(rows_ref, hold, own_sems.at[0])
    own.start()
    own.wait()
    own = pltpu.make_async_copy(hold, out_ref.at[tp, me], own_sems.at[1])
    own.start()
    own.wait()
    for k in range(1, group):
        owner = (me + group - k) % group
        across(k, owner).wait_recv()
        for j in range(1, tp_count):
            beside(j, k, out_ref.at[tp, owner], tp, owner).start()
    for k in range(1, group):
        across(k, me).wait_send()
    for j in range(1, tp_count):
        for k in range(group):
            owner = (me + group - k) % group
            copy = beside(j, k, rows_ref, (tp + tp_count - j) % tp_count, owner)
            copy.wait_send()
            copy.wait_recv()


def gather_rows(rows):
    group = group_size(lax.axis_size("sp"))
    tp_count = lax.axis_size("tp")
    return pl.pallas_call(
        functools.partial(gather_kernel, group, tp_count),
        out_shape=jax.ShapeDtypeStruct((tp_count, group) + rows.shape, rows.dtype),
        in_specs=[pl.BlockSpec(memory_space=pl.ANY)],
        out_specs=pl.BlockSpec(memory_space=pl.ANY),
        scratch_shapes=[
            pltpu.VMEM(rows.shape, rows.dtype),
            pltpu.SemaphoreType.DMA((2, group)),
            pltpu.SemaphoreType.DMA((2,)),
            pltpu.SemaphoreType.DMA((2, tp_count, group)),
        ],
        compiler_params=pltpu.CompilerParams(collective_id=1, has_side_effects=True),
    )(rows)


def return_kernel(group, parts_ref, out_ref, hold, sems, own_sems):
    sp = lax.axis_index("sp")
    base = (sp // group) * group
    me = sp - base
    barrier = pltpu.get_barrier_semaphore()
    for k in range(1, group):
        pl.semaphore_signal(
            barrier,
            inc=1,
            device_id={"sp": base + (me + k) % group},
            device_id_type=pl.DeviceIdType.MESH,
        )
    pl.semaphore_wait(barrier, group - 1)

    def across(k, owner):
        peer = (me + k) % group
        return pltpu.make_async_remote_copy(
            src_ref=parts_ref.at[peer],
            dst_ref=out_ref.at[owner],
            send_sem=sems.at[0, k],
            recv_sem=sems.at[1, k],
            device_id={"sp": base + peer},
            device_id_type=pl.DeviceIdType.MESH,
        )

    for k in range(1, group):
        across(k, me).start()
    own = pltpu.make_async_copy(parts_ref.at[me], hold, own_sems.at[0])
    own.start()
    own.wait()
    own = pltpu.make_async_copy(hold, out_ref.at[me], own_sems.at[1])
    own.start()
    own.wait()
    for k in range(1, group):
        copy = across(k, (me + group - k) % group)
        copy.wait_recv()
        copy.wait_send()


def return_parts(parts):
    group = parts.shape[0]
    return pl.pallas_call(
        functools.partial(return_kernel, group),
        out_shape=jax.ShapeDtypeStruct(parts.shape, parts.dtype),
        in_specs=[pl.BlockSpec(memory_space=pl.ANY)],
        out_specs=pl.BlockSpec(memory_space=pl.ANY),
        scratch_shapes=[
            pltpu.VMEM(parts.shape[1:], parts.dtype),
            pltpu.SemaphoreType.DMA((2, group)),
            pltpu.SemaphoreType.DMA((2,)),
        ],
        compiler_params=pltpu.CompilerParams(collective_id=2, has_side_effects=True),
    )(parts)


def local(
    residual,
    queries_narrow,
    keys_narrow,
    values_narrow,
    queries_broad,
    keys_broad,
    values_broad,
    gates_narrow,
    gates_broad,
    project_narrow,
    project_broad,
    norm_gain,
    up_weight,
    down_weight,
):
    local_count = queries_narrow.shape[0]
    up_full, down_full = share_weights(up_weight, down_weight)
    table_narrow, table_broad = (
        lax.all_gather(gates_narrow, "sp", axis=0, tiled=True),
        lax.all_gather(gates_broad, "sp", axis=0, tiled=True),
    )
    query_pos = lax.axis_index("sp") * local_count + jnp.arange(local_count, dtype=jnp.int32)
    initial = (
        empty_state(local_count, queries_narrow.shape[1] // A_DIM, A_DIM),
        empty_state(local_count, queries_broad.shape[1] // B_DIM, B_DIM),
    )
    piece_keys_narrow = lax.all_gather(keys_narrow, "sp", axis=0, tiled=True)
    piece_values_narrow = lax.all_gather(values_narrow, "sp", axis=0, tiled=True)
    piece_keys_broad = lax.all_gather(keys_broad, "sp", axis=0, tiled=True)
    piece_values_broad = lax.all_gather(values_broad, "sp", axis=0, tiled=True)
    piece_count = piece_keys_narrow.shape[0]
    key_pos = jnp.arange(piece_count, dtype=jnp.int32)
    allowed = key_pos[None, :] <= query_pos[:, None]
    state_narrow = group_update(
        initial[0],
        queries_narrow,
        piece_keys_narrow,
        piece_values_narrow,
        gates_narrow,
        table_narrow,
        allowed,
        A_DIM,
    )
    state_broad = group_update(
        initial[1],
        queries_broad,
        piece_keys_broad,
        piece_values_broad,
        gates_broad,
        table_broad,
        allowed,
        B_DIM,
    )
    attended_narrow = finish_group(state_narrow, A_DIM)
    attended_broad = finish_group(state_broad, B_DIM)
    projected = lax.psum_scatter(
        (
            jnp.dot(attended_narrow, project_narrow, preferred_element_type=jnp.float32)
            + jnp.dot(attended_broad, project_broad, preferred_element_type=jnp.float32)
        ).astype(jnp.bfloat16),
        "tp",
        scatter_dimension=0,
        tiled=True,
    ).astype(jnp.float32)
    mixed = (residual.astype(jnp.float32) + projected).astype(jnp.bfloat16)
    features = gather_rows(rms_scaled(mixed, norm_gain))
    tp_count, group, rows, width = features.shape
    up_total = jnp.dot(
        features.reshape(tp_count * group * rows, width),
        up_full,
        preferred_element_type=jnp.float32,
    )
    hidden = jnp.square(jax.nn.relu(up_total)).astype(jnp.bfloat16)
    down_term = jnp.dot(hidden, down_full, preferred_element_type=jnp.float32)
    parts = lax.psum_scatter(
        down_term.astype(jnp.bfloat16).reshape(features.shape),
        "tp",
        scatter_dimension=0,
        tiled=False,
    )
    summed_rows = jnp.sum(return_parts(parts).astype(jnp.float32), axis=0)
    return (mixed.astype(jnp.float32) + summed_rows).astype(jnp.bfloat16)


def solution(mesh):
    return jax.shard_map(
        local,
        mesh=mesh,
        in_specs=(
            P(("sp", "tp"), None),
            P("sp", "tp"),
            P("sp", "tp"),
            P("sp", "tp"),
            P("sp", "tp"),
            P("sp", "tp"),
            P("sp", "tp"),
            P("sp", "tp"),
            P("sp", "tp"),
            P("tp", None),
            P("tp", None),
            P(),
            P("sp", "tp"),
            P("tp", "sp"),
        ),
        out_specs=P(("sp", "tp"), None),
        check_vma=False,
    )
```

```python
import functools

import jax
import jax.numpy as jnp
from jax import lax
from jax.experimental import pallas as pl
from jax.experimental.pallas import tpu as pltpu
from jax.sharding import PartitionSpec as P

A_DIM = 32
B_DIM = 64


def rms_scaled(mixed, norm_gain):
    mixed_wide = mixed.astype(jnp.float32)
    scale = lax.rsqrt(jnp.mean(mixed_wide * mixed_wide, axis=-1, keepdims=True) + 1e-06)
    return (mixed_wide * scale * norm_gain).astype(jnp.bfloat16)


def group_size(sp_count):
    return 8 if sp_count % 8 == 0 else sp_count


def head_columns(narrow_heads):
    ranges = [(h * A_DIM, (h + 1) * A_DIM, A_DIM) for h in range(narrow_heads)]
    return ranges + [(narrow_heads * A_DIM, narrow_heads * A_DIM + B_DIM, B_DIM)]


def attend_block(ranges, block, query, kv_all, gate_all):
    tokens, width = query.shape
    lane = lax.broadcasted_iota(jnp.int32, (tokens, width), 1)
    row = lax.broadcasted_iota(jnp.int32, (tokens, tokens), 0)
    column = lax.broadcasted_iota(jnp.int32, (tokens, tokens), 1)
    inside = [(lane >= low) & (lane < high) for low, high, _ in ranges]
    wide = query.astype(jnp.float32)
    head_queries = [jnp.where(mask, wide, 0.0).astype(jnp.bfloat16) for mask in inside]
    own_gates = gate_all[block]
    query_gates = [
        jnp.sum(jnp.where(row == column, own_gates[h : h + 1, :], 0.0), axis=1, keepdims=True)
        for h in range(len(ranges))
    ]

    def by_head(columns):
        spread = jnp.broadcast_to(columns[-1], (tokens, width))
        for mask, values in zip(inside[:-1], columns[:-1]):
            spread = jnp.where(mask, values, spread)
        return spread

    def step(key_block, state):
        peaks, totals, summed = state
        keys = kv_all[key_block, :, :width]
        values = kv_all[key_block, :, width:]
        key_gates = gate_all[key_block]
        allowed = column + (key_block - block) * tokens <= row
        new_peaks, new_totals, fades, terms = [], [], [], []
        for h, (_, _, size) in enumerate(ranges):
            scores = (
                lax.dot_general(
                    head_queries[h],
                    keys,
                    (((1,), (1,)), ((), ())),
                    preferred_element_type=jnp.float32,
                )
                * size ** (-0.5)
                + query_gates[h]
                - key_gates[h : h + 1, :]
            )
            scores = jnp.where(allowed, scores, -1e30)
            peak = jnp.maximum(peaks[h], jnp.max(scores, axis=1, keepdims=True))
            weights = jnp.exp(scores - peak)
            fade = jnp.exp(peaks[h] - peak)
            new_peaks.append(peak)
            new_totals.append(totals[h] * fade + jnp.sum(weights, axis=1, keepdims=True))
            fades.append(fade)
            terms.append(
                jnp.dot(
                    weights.astype(jnp.bfloat16), values, preferred_element_type=jnp.float32
                )
            )
        summed = summed * by_head(fades) + by_head(terms)
        return tuple(new_peaks), tuple(new_totals), summed

    heads = len(ranges)
    initial = (
        tuple(jnp.full((tokens, 1), -1e30, jnp.float32) for _ in range(heads)),
        tuple(jnp.zeros((tokens, 1), jnp.float32) for _ in range(heads)),
        jnp.zeros((tokens, width), jnp.float32),
    )
    _, totals, summed = lax.fori_loop(0, block + 1, step, initial)
    return (summed / by_head(totals)).astype(jnp.bfloat16)


def layer_kernel(
    count,
    group,
    ranges,
    q_ref,
    kv_ref,
    gate_ref,
    up_ref,
    down_ref,
    attended_out,
    up_out,
    down_out,
    q_all,
    kv_all,
    gate_all,
    attended,
    up_hold,
    down_hold,
    kv_sems,
    gate_sems,
    q_sems,
    back_sems,
    sems,
    own_sems,
):
    me = lax.axis_index("sp")
    head_groups = q_ref.shape[0]
    parts = count // head_groups
    my_heads = me % head_groups
    my_part = me // head_groups

    def block_of(part, slot):
        turn = slot % 2
        return slot * parts + (1 - turn) * part + turn * (parts - 1 - part)

    my_slot = me // parts
    my_turn = my_slot % 2
    place = me % parts
    reader_part = (1 - my_turn) * place + my_turn * (parts - 1 - place)
    up_rows = up_ref.shape[0]
    units = up_out.shape[1]
    columns = down_ref.shape[1]
    barrier = pltpu.get_barrier_semaphore()

    def hello(k, carry):
        pl.semaphore_signal(
            barrier,
            inc=1,
            device_id={"sp": (me + k) % count},
            device_id_type=pl.DeviceIdType.MESH,
        )
        return carry

    lax.fori_loop(1, count, hello, 0)
    pl.semaphore_wait(barrier, count - 1)

    def remote(source, target, sem_pair, first, second, peer):
        return pltpu.make_async_remote_copy(
            src_ref=source,
            dst_ref=target,
            send_sem=sem_pair.at[0, first],
            recv_sem=sem_pair.at[1, second],
            device_id={"sp": peer},
            device_id_type=pl.DeviceIdType.MESH,
        )

    def context_copies(k, owner):
        peer = (me + k) % count
        heads = peer % head_groups
        return (
            remote(kv_ref.at[heads], kv_all.at[owner], kv_sems, k, k, peer),
            remote(gate_ref.at[heads], gate_all.at[owner], gate_sems, k, k, peer),
        )

    def start_context(k, carry):
        for copy in context_copies(k, me):
            copy.start()
        return carry

    def wait_context(k, carry):
        for copy in context_copies(k, (me + count - k) % count):
            copy.wait_recv()
            copy.wait_send()
        return carry

    for heads in range(head_groups):
        reader = reader_part * head_groups + heads

        @pl.when(reader != me)
        def _():
            remote(q_ref.at[heads], q_all.at[my_slot], q_sems, heads, my_slot, reader).start()

        @pl.when(reader == me)
        def _():
            q_all[my_slot] = q_ref[heads]

    lax.fori_loop(1, count, start_context, 0)
    kv_all[me] = kv_ref[my_heads]
    gate_all[me] = gate_ref[my_heads]

    def up_source(chunk):
        return up_ref.at[:, pl.ds(pl.multiple_of(chunk * units, 128), units)]

    def down_source(chunk):
        return down_ref.at[pl.ds(pl.multiple_of(chunk * units, units), units), :]

    def up_target(owner):
        return up_out.at[pl.ds(pl.multiple_of(owner * up_rows, up_rows), up_rows), :]

    def down_target(owner):
        if len(down_out.shape) == 3:
            return down_out.at[owner]
        return down_out.at[:, pl.ds(pl.multiple_of(owner * columns, columns), columns)]

    def copies(k, target_owner):
        peer = (me + k) % count
        chunk = peer % group
        pairs = (
            (up_source(chunk), up_target(target_owner)),
            (down_source(chunk), down_target(target_owner)),
        )
        return [
            pltpu.make_async_remote_copy(
                src_ref=source,
                dst_ref=target,
                send_sem=sems.at[0, which, k],
                recv_sem=sems.at[1, which, k],
                device_id={"sp": peer},
                device_id_type=pl.DeviceIdType.MESH,
            )
            for which, (source, target) in enumerate(pairs)
        ]

    def start(k, carry):
        for copy in copies(k, me):
            copy.start()
        return carry

    def finish(k, carry):
        for copy in copies(k, (me + count - k) % count):
            copy.wait_recv()
            copy.wait_send()
        return carry

    lax.fori_loop(1, count, start, 0)
    own = me % group
    first = [
        pltpu.make_async_copy(up_source(own), up_hold, own_sems.at[0]),
        pltpu.make_async_copy(down_source(own), down_hold, own_sems.at[1]),
    ]
    for copy in first:
        copy.start()
    for copy in first:
        copy.wait()
    second = [
        pltpu.make_async_copy(up_hold, up_target(me), own_sems.at[0]),
        pltpu.make_async_copy(down_hold, down_target(me), own_sems.at[1]),
    ]
    for copy in second:
        copy.start()
    for heads in range(head_groups):
        reader = reader_part * head_groups + heads

        @pl.when(reader != me)
        def _():
            remote(q_ref.at[heads], q_all.at[my_slot], q_sems, heads, my_slot, reader).wait_send()

    for slot in range(head_groups):
        owner = block_of(my_part, slot)

        @pl.when(owner != me)
        def _():
            remote(q_ref.at[0], q_all.at[slot], q_sems, 0, slot, owner).wait_recv()

    lax.fori_loop(1, count, wait_context, 0)

    def attend(slot, carry):
        block = block_of(my_part, slot)
        attended[slot] = attend_block(ranges, block, q_all[slot], kv_all, gate_all)
        return carry

    lax.fori_loop(0, head_groups, attend, 0)
    for slot in range(head_groups):
        owner = block_of(my_part, slot)

        @pl.when(owner != me)
        def _():
            remote(
                attended.at[slot], attended_out.at[my_heads], back_sems, slot, my_heads, owner
            ).start()

        @pl.when(owner == me)
        def _():
            attended_out[my_heads] = attended[slot]

    for copy in second:
        copy.wait()
    lax.fori_loop(1, count, finish, 0)
    for slot in range(head_groups):
        owner = block_of(my_part, slot)

        @pl.when(owner != me)
        def _():
            remote(
                attended.at[slot], attended_out.at[my_heads], back_sems, slot, my_heads, owner
            ).wait_send()

    for heads in range(head_groups):
        reader = reader_part * head_groups + heads

        @pl.when(reader != me)
        def _():
            remote(
                attended.at[0], attended_out.at[heads], back_sems, 0, heads, reader
            ).wait_recv()


def attend_and_share(queries, keys_values, gates, ranges, up_weight, down_weight):
    head_groups, tokens, head_width = queries.shape
    count = lax.axis_size("sp")
    group = group_size(count)
    up_rows, unit_total = up_weight.shape
    columns = down_weight.shape[1]
    units = unit_total // group
    if columns % 128 == 0:
        down_shape = (units, count * columns)
    else:
        down_shape = (count, units, columns)
    attended, up_full, down_full = pl.pallas_call(
        functools.partial(layer_kernel, count, group, ranges),
        out_shape=(
            jax.ShapeDtypeStruct(queries.shape, queries.dtype),
            jax.ShapeDtypeStruct((count * up_rows, units), up_weight.dtype),
            jax.ShapeDtypeStruct(down_shape, down_weight.dtype),
        ),
        in_specs=[pl.BlockSpec(memory_space=pltpu.VMEM)] * 3
        + [pl.BlockSpec(memory_space=pl.ANY)] * 2,
        out_specs=[pl.BlockSpec(memory_space=pltpu.VMEM)]
        + [pl.BlockSpec(memory_space=pl.ANY)] * 2,
        scratch_shapes=[
            pltpu.VMEM(queries.shape, queries.dtype),
            pltpu.VMEM((count,) + keys_values.shape[1:], keys_values.dtype),
            pltpu.VMEM((count,) + gates.shape[1:], gates.dtype),
            pltpu.VMEM(queries.shape, queries.dtype),
            pltpu.VMEM((up_rows, units), up_weight.dtype),
            pltpu.VMEM((units, columns), down_weight.dtype),
            pltpu.SemaphoreType.DMA((2, count)),
            pltpu.SemaphoreType.DMA((2, count)),
            pltpu.SemaphoreType.DMA((2, head_groups)),
            pltpu.SemaphoreType.DMA((2, head_groups)),
            pltpu.SemaphoreType.DMA((2, 2, count)),
            pltpu.SemaphoreType.DMA((2,)),
        ],
        compiler_params=pltpu.CompilerParams(collective_id=0, has_side_effects=True),
        cost_estimate=pl.CostEstimate(
            flops=0, bytes_accessed=count * up_rows * units * 80, transcendentals=0
        ),
    )(queries, keys_values, gates, up_weight, down_weight)
    if columns % 128:
        down_full = down_full.transpose(1, 0, 2).reshape(units, count * columns)
    return attended, up_full, down_full


def gather_kernel(group, tp_count, rows_ref, out_ref, hold, sems, own_sems, pass_sems):
    sp = lax.axis_index("sp")
    tp = lax.axis_index("tp")
    base = (sp // group) * group
    me = sp - base
    barrier = pltpu.get_barrier_semaphore()
    for k in range(1, group):
        pl.semaphore_signal(
            barrier,
            inc=1,
            device_id={"sp": base + (me + k) % group},
            device_id_type=pl.DeviceIdType.MESH,
        )
    for j in range(1, tp_count):
        pl.semaphore_signal(
            barrier,
            inc=1,
            device_id={"tp": (tp + j) % tp_count},
            device_id_type=pl.DeviceIdType.MESH,
        )
    pl.semaphore_wait(barrier, group + tp_count - 2)

    def across(k, owner):
        return pltpu.make_async_remote_copy(
            src_ref=rows_ref,
            dst_ref=out_ref.at[tp, owner],
            send_sem=sems.at[0, k],
            recv_sem=sems.at[1, k],
            device_id={"sp": base + (me + k) % group},
            device_id_type=pl.DeviceIdType.MESH,
        )

    def beside(j, k, source, tp_owner, owner):
        return pltpu.make_async_remote_copy(
            src_ref=source,
            dst_ref=out_ref.at[tp_owner, owner],
            send_sem=pass_sems.at[0, j, k],
            recv_sem=pass_sems.at[1, j, k],
            device_id={"tp": (tp + j) % tp_count},
            device_id_type=pl.DeviceIdType.MESH,
        )

    for k in range(1, group):
        across(k, me).start()
    for j in range(1, tp_count):
        beside(j, 0, rows_ref, tp, me).start()
    own = pltpu.make_async_copy(rows_ref, hold, own_sems.at[0])
    own.start()
    own.wait()
    own = pltpu.make_async_copy(hold, out_ref.at[tp, me], own_sems.at[1])
    own.start()
    own.wait()
    for k in range(1, group):
        owner = (me + group - k) % group
        across(k, owner).wait_recv()
        for j in range(1, tp_count):
            beside(j, k, out_ref.at[tp, owner], tp, owner).start()
    for k in range(1, group):
        across(k, me).wait_send()
    for j in range(1, tp_count):
        for k in range(group):
            owner = (me + group - k) % group
            copy = beside(j, k, rows_ref, (tp + tp_count - j) % tp_count, owner)
            copy.wait_send()
            copy.wait_recv()


def gather_rows(rows):
    group = group_size(lax.axis_size("sp"))
    tp_count = lax.axis_size("tp")
    return pl.pallas_call(
        functools.partial(gather_kernel, group, tp_count),
        out_shape=jax.ShapeDtypeStruct((tp_count, group) + rows.shape, rows.dtype),
        in_specs=[pl.BlockSpec(memory_space=pl.ANY)],
        out_specs=pl.BlockSpec(memory_space=pl.ANY),
        scratch_shapes=[
            pltpu.VMEM(rows.shape, rows.dtype),
            pltpu.SemaphoreType.DMA((2, group)),
            pltpu.SemaphoreType.DMA((2,)),
            pltpu.SemaphoreType.DMA((2, tp_count, group)),
        ],
        compiler_params=pltpu.CompilerParams(collective_id=1, has_side_effects=True),
    )(rows)


def return_kernel(group, parts_ref, out_ref, hold, sems, own_sems):
    sp = lax.axis_index("sp")
    base = (sp // group) * group
    me = sp - base
    barrier = pltpu.get_barrier_semaphore()
    for k in range(1, group):
        pl.semaphore_signal(
            barrier,
            inc=1,
            device_id={"sp": base + (me + k) % group},
            device_id_type=pl.DeviceIdType.MESH,
        )
    pl.semaphore_wait(barrier, group - 1)

    def across(k, owner):
        peer = (me + k) % group
        return pltpu.make_async_remote_copy(
            src_ref=parts_ref.at[peer],
            dst_ref=out_ref.at[owner],
            send_sem=sems.at[0, k],
            recv_sem=sems.at[1, k],
            device_id={"sp": base + peer},
            device_id_type=pl.DeviceIdType.MESH,
        )

    for k in range(1, group):
        across(k, me).start()
    own = pltpu.make_async_copy(parts_ref.at[me], hold, own_sems.at[0])
    own.start()
    own.wait()
    own = pltpu.make_async_copy(hold, out_ref.at[me], own_sems.at[1])
    own.start()
    own.wait()
    for k in range(1, group):
        copy = across(k, (me + group - k) % group)
        copy.wait_recv()
        copy.wait_send()


def return_parts(parts):
    group = parts.shape[0]
    return pl.pallas_call(
        functools.partial(return_kernel, group),
        out_shape=jax.ShapeDtypeStruct(parts.shape, parts.dtype),
        in_specs=[pl.BlockSpec(memory_space=pl.ANY)],
        out_specs=pl.BlockSpec(memory_space=pl.ANY),
        scratch_shapes=[
            pltpu.VMEM(parts.shape[1:], parts.dtype),
            pltpu.SemaphoreType.DMA((2, group)),
            pltpu.SemaphoreType.DMA((2,)),
        ],
        compiler_params=pltpu.CompilerParams(collective_id=2, has_side_effects=True),
    )(parts)


def local(
    residual,
    queries_narrow,
    keys_narrow,
    values_narrow,
    queries_broad,
    keys_broad,
    values_broad,
    gates_narrow,
    gates_broad,
    project_narrow,
    project_broad,
    norm_gain,
    up_weight,
    down_weight,
):
    tokens = queries_narrow.shape[0]
    head_groups = gates_broad.shape[1]
    narrow_heads = gates_narrow.shape[1] // head_groups
    ranges = head_columns(narrow_heads)

    def by_group(narrow, broad):
        return jnp.concatenate(
            [part.reshape(tokens, head_groups, -1) for part in (narrow, broad)], axis=-1
        ).transpose(1, 0, 2)

    gates = jnp.concatenate(
        [gates_narrow.reshape(tokens, head_groups, narrow_heads), gates_broad[..., None]], axis=-1
    ).transpose(1, 2, 0)
    gates = jnp.pad(gates, ((0, 0), (0, -gates.shape[1] % 8), (0, 0)))
    attended, up_full, down_full = attend_and_share(
        by_group(queries_narrow, queries_broad),
        jnp.concatenate(
            [by_group(keys_narrow, keys_broad), by_group(values_narrow, values_broad)], axis=-1
        ),
        gates,
        ranges,
        up_weight,
        down_weight,
    )
    rows_first = attended.transpose(1, 0, 2)
    split = narrow_heads * A_DIM
    attended_narrow = rows_first[..., :split].reshape(tokens, -1)
    attended_broad = rows_first[..., split:].reshape(tokens, -1)
    projected = lax.psum_scatter(
        (
            jnp.dot(attended_narrow, project_narrow, preferred_element_type=jnp.float32)
            + jnp.dot(attended_broad, project_broad, preferred_element_type=jnp.float32)
        ).astype(jnp.bfloat16),
        "tp",
        scatter_dimension=0,
        tiled=True,
    ).astype(jnp.float32)
    mixed = (residual.astype(jnp.float32) + projected).astype(jnp.bfloat16)
    features = gather_rows(rms_scaled(mixed, norm_gain))
    tp_count, group, rows, width = features.shape
    up_total = jnp.dot(
        features.reshape(tp_count * group * rows, width),
        up_full,
        preferred_element_type=jnp.float32,
    )
    hidden = jnp.square(jax.nn.relu(up_total)).astype(jnp.bfloat16)
    down_term = jnp.dot(hidden, down_full, preferred_element_type=jnp.float32)
    parts = lax.psum_scatter(
        down_term.astype(jnp.bfloat16).reshape(features.shape),
        "tp",
        scatter_dimension=0,
        tiled=False,
    )
    summed_rows = jnp.sum(return_parts(parts).astype(jnp.float32), axis=0)
    return (mixed.astype(jnp.float32) + summed_rows).astype(jnp.bfloat16)


def solution(mesh):
    return jax.shard_map(
        local,
        mesh=mesh,
        in_specs=(
            P(("sp", "tp"), None),
            P("sp", "tp"),
            P("sp", "tp"),
            P("sp", "tp"),
            P("sp", "tp"),
            P("sp", "tp"),
            P("sp", "tp"),
            P("sp", "tp"),
            P("sp", "tp"),
            P("tp", None),
            P("tp", None),
            P(),
            P("sp", "tp"),
            P("tp", "sp"),
        ),
        out_specs=P(("sp", "tp"), None),
        check_vma=False,
    )
```
